32 devices in a mesh: sp: 16 (over z, y, x), tp: 2 (over core).
Axes of the slice: x: 2, y: 2, z: 4, core: 2. Of those that a mesh axis runs over, the one named last changes fastest.
Arguments:
- query_proj: bfloat16 [4096, 1024], P('sp', 'tp'), may hold values from -6 to 6
- key_proj: bfloat16 [4096, 512], P('sp', 'tp'), may hold values from -6 to 6
- value_proj: bfloat16 [4096, 512], P('sp', 'tp'), may hold values from -6 to 6
- q_gain: float32 [64], replicated, may hold values from 1.1 to 10, as said below
- k_gain: float32 [64], replicated, may hold values from 1.1 to 10, as said below
- residual: bfloat16 [4096, 2048], P('sp'), may hold values from -6 to 6
- out_weight: bfloat16 [1024, 2048], P('tp'), may hold values from -0.75 to 0.75
- norm_gain: float32 [2048], replicated, may hold values from 0.1 to 1.9
- value_weight: bfloat16 [2048, 5120], P('sp', 'tp'), may hold values from -0.125 to 0.125
- gate_weight: bfloat16 [2048, 5120], P('sp', 'tp'), may hold values from -0.125 to 0.125
- down_weight: bfloat16 [5120, 2048], P('tp', 'sp'), may hold values from -0.078125 to 0.078125
- conv_value: float32 [3, 5120], P(None, 'tp'), may hold values from -3.5 to 3.5
- conv_gate: float32 [3, 5120], P(None, 'tp'), may hold values from -3.5 to 3.5
Outputs:
- layer_out: bfloat16 [4096, 2048], P(('sp', 'tp'))
The draws below stay inside these ranges and needn't reach their ends.
Inputs may be any that keep to these rules, and one draw needn't show every extreme that they name: `q_gain`: per-dimension gains of the query norm. `k_gain`: per-dimension gains of the key norm.
All inputs are finite; a program needn't handle non-finite values.
Results may differ from the reference program's by a relative error of at most 0.015.
The reference program's roundings to bfloat16 on the way count: a program that leaves them out, or rounds other values in their place, can miss the bound.
Values may be sent and summed in bfloat16 or wider, within the bound.
No kernel may reach another device: no remote copies, remote signals or barrier semaphores. Data moves between devices by JAX's collectives and lax.ppermute only.
A program may use at most 128 MiB of HBM per device.

```python
import math
import jax
import jax.numpy as jnp
from jax import lax

D = 2048
HEADS = 16
KV_HEADS = 8
HEAD_DIM = 64
FF = 5120
GRID_W = 64
CONV_W = 3
SEQ = 4096
N_TP = 2


def gain_draw(key, salt_value):
    key_here = jax.random.fold_in(key, salt_value)
    return jnp.exp(jax.random.uniform(key_here, (HEAD_DIM,), jnp.float32, jnp.log(1.1), jnp.log(2.0)))


def draw_q_gain(key, part):
    return gain_draw(key, 11)


def draw_k_gain(key, part):
    return gain_draw(key, 23)


def block_scale(key, dims, pieces, least, top_value):
    gain, own = 1.0, jax.random.fold_in(key, 6)
    for axis_at, parts in pieces:
        steps = jnp.exp(jax.random.uniform(jax.random.fold_in(own, axis_at), (parts,), jnp.float32, least / len(pieces), top_value / len(pieces)))
        gain = gain * jnp.repeat(steps, dims[axis_at] // parts).reshape([-1 if axis == axis_at else 1 for axis in range(len(dims))])
    return gain


def centred(rng, extent, width, limit, cuts=(), kind=jnp.bfloat16):
    result = width * jax.random.normal(rng, extent, jnp.float32)
    if cuts:
        result = result * block_scale(rng, extent, cuts, -0.22, 0.18)
    return jnp.clip(result, -limit, limit).astype(kind)


def setup_inputs(seed: int = 0) -> dict:
    splits = jax.random.split(jax.random.key(seed), 14)
    query_proj = centred(splits[0], (SEQ, HEADS * HEAD_DIM), 1.0, 6.0, ((0, 16), (1, 2)))
    key_proj = centred(splits[1], (SEQ, KV_HEADS * HEAD_DIM), 1.0, 6.0, ((0, 16), (1, 2)))
    value_proj = centred(splits[2], (SEQ, KV_HEADS * HEAD_DIM), 1.0, 6.0, ((0, 16), (1, 2)))
    q_gain = draw_q_gain(jax.random.fold_in(splits[13], 71), 0)
    k_gain = draw_k_gain(jax.random.fold_in(splits[13], 71), 0)
    residual = centred(splits[5], (SEQ, D), 1.0, 6.0, ((0, 16),))
    out_weight = centred(splits[6], (HEADS * HEAD_DIM, D), (HEADS * HEAD_DIM // 16) ** -0.5, 0.75, ((0, 2),))
    norm_gain = jnp.clip(1.0 + 0.18 * jax.random.normal(splits[7], (D,), jnp.float32), 0.1, 1.9)
    value_weight = centred(splits[8], (D, FF), D ** -0.5, 0.125, ((0, 16), (1, 2)))
    gate_weight = centred(splits[9], (D, FF), D ** -0.5, 0.125, ((0, 16), (1, 2)))
    down_weight = centred(splits[10], (FF, D), FF ** -0.5, 0.078125, ((0, 2), (1, 16)))
    conv_value = centred(splits[11], (CONV_W, FF), CONV_W ** -0.5, 3.5, ((1, 2),), jnp.float32)
    conv_gate = centred(splits[12], (CONV_W, FF), CONV_W ** -0.5, 3.5, ((1, 2),), jnp.float32)
    return {"query_proj": query_proj, "key_proj": key_proj, "value_proj": value_proj, "q_gain": q_gain, "k_gain": k_gain, "residual": residual, "out_weight": out_weight, "norm_gain": norm_gain, "value_weight": value_weight, "gate_weight": gate_weight, "down_weight": down_weight, "conv_value": conv_value, "conv_gate": conv_gate}


NORM_EPS = 1e-06
ROPE_BASE = 10000.0

def rms_norm(block_in, gain_vec):
    values = block_in.astype(jnp.float32)
    inv_rms = lax.rsqrt(lax.optimization_barrier(jnp.mean(values * values, axis=-1, keepdims=True)) + NORM_EPS)
    return values * inv_rms * gain_vec.astype(jnp.float32)

def rotate_half(values, position):
    full_width = values.shape[-1]
    half_width = full_width // 2
    frequency = ROPE_BASE ** (-jnp.arange(0, full_width, 2, dtype=jnp.float32) / full_width)
    angles = position.astype(jnp.float32)[:, None] * frequency[None, :]
    cosine = jnp.cos(angles)[:, None, :]
    sine_part = jnp.sin(angles)[:, None, :]
    first_half = values[..., :half_width]
    second_half = values[..., half_width:]
    return jnp.concatenate([first_half * cosine - second_half * sine_part, first_half * sine_part + second_half * cosine], axis=-1)

def grid_rotary(values, positions):
    half_width = values.shape[-1] // 2
    grid_row = positions // GRID_W
    column = positions % GRID_W
    return jnp.concatenate([rotate_half(values[..., :half_width], grid_row), rotate_half(values[..., half_width:], column)], axis=-1)

def depthwise(up_rows, tap_weights):
    padded = jnp.pad(up_rows.astype(jnp.float32), ((1, 1), (0, 0)))
    weights = tap_weights.astype(jnp.float32)
    return padded[:-2] * weights[0] + padded[1:-1] * weights[1] + padded[2:] * weights[2]

def reference(query_proj, key_proj, value_proj, q_gain, k_gain, residual, out_weight, norm_gain, value_weight, gate_weight, down_weight, conv_value, conv_gate):
    sequence = query_proj.shape[0]
    positions = jnp.arange(sequence, dtype=jnp.int32)
    group_size = HEADS // KV_HEADS
    queries = grid_rotary(rms_norm(query_proj.reshape(sequence, HEADS, HEAD_DIM), q_gain), positions) * HEAD_DIM ** (-0.5)
    queries = lax.optimization_barrier(queries.astype(jnp.bfloat16)).astype(jnp.float32)
    keys_rot = grid_rotary(rms_norm(key_proj.reshape(sequence, KV_HEADS, HEAD_DIM), k_gain), positions)
    keys_rot = lax.optimization_barrier(keys_rot.astype(jnp.bfloat16)).astype(jnp.float32)
    keys_rep = jnp.repeat(keys_rot, group_size, axis=1)
    values_rep = jnp.repeat(value_proj.reshape(sequence, KV_HEADS, HEAD_DIM).astype(jnp.float32), group_size, axis=1)
    q_span = math.gcd(sequence, 256)

    def attend(q_block):
        scores = jnp.einsum('qhd,shd->hqs', q_block, keys_rep)
        row_max = lax.optimization_barrier(jnp.max(scores, axis=-1, keepdims=True))
        weights = jnp.exp(scores - row_max)
        totals = lax.optimization_barrier(jnp.sum(weights, axis=-1))
        rounded = lax.optimization_barrier(weights.astype(jnp.bfloat16)).astype(jnp.float32)
        summed = jnp.einsum('hqs,shd->qhd', rounded, values_rep)
        return summed / jnp.transpose(totals)[:, :, None]
    results = lax.map(attend, queries.reshape(sequence // q_span, q_span, HEADS, HEAD_DIM))
    attended = results.reshape(sequence, HEADS * HEAD_DIM).astype(jnp.bfloat16)
    head_cols = HEADS * HEAD_DIM // N_TP
    mix_sum = jnp.zeros((sequence, D), jnp.float32)
    for group_index in range(N_TP):
        partial_sum = jnp.dot(attended[:, group_index * head_cols:(group_index + 1) * head_cols], out_weight[group_index * head_cols:(group_index + 1) * head_cols], preferred_element_type=jnp.float32)
        mix_sum = mix_sum + lax.optimization_barrier(partial_sum.astype(jnp.bfloat16)).astype(jnp.float32)
    mix_out = mix_sum.astype(jnp.bfloat16)
    updated = (residual.astype(jnp.float32) + mix_out.astype(jnp.float32)).astype(jnp.bfloat16)
    normed = rms_norm(updated, norm_gain).astype(jnp.bfloat16)
    value_up = jnp.dot(normed, value_weight, preferred_element_type=jnp.float32).astype(jnp.bfloat16)
    gate_up = jnp.dot(normed, gate_weight, preferred_element_type=jnp.float32).astype(jnp.bfloat16)
    conv_val = depthwise(value_up, conv_value)
    conv_gated = depthwise(gate_up, conv_gate)
    hidden = (jax.nn.gelu(conv_gated, approximate=True) * conv_val).astype(jnp.bfloat16)
    ff_cols = FF // N_TP
    branch_sum = jnp.zeros((sequence, D), jnp.float32)
    for group_index in range(N_TP):
        partial_sum = jnp.dot(hidden[:, group_index * ff_cols:(group_index + 1) * ff_cols], down_weight[group_index * ff_cols:(group_index + 1) * ff_cols], preferred_element_type=jnp.float32)
        branch_sum = branch_sum + lax.optimization_barrier(partial_sum.astype(jnp.bfloat16)).astype(jnp.float32)
    branch = branch_sum.astype(jnp.bfloat16)
    return (updated.astype(jnp.float32) + branch.astype(jnp.float32)).astype(jnp.bfloat16)
```

```python
import functools

import jax
import jax.numpy as jnp
from jax import lax
from jax.experimental import pallas as pl
from jax.experimental.pallas import tpu as pltpu
from jax.sharding import PartitionSpec as P

HEAD_DIM = 64
GRID_W = 64
LANES = 128

NORM_EPS = 1e-06
ROPE_BASE = 10000.0


A_BITS = (0, 2)
B_BITS = (1, 3)

F32 = jnp.float32
BF16 = jnp.bfloat16


def spread(index, bits):
    return sum(((index >> i) & 1) << b for i, b in enumerate(bits))


A_MASKS = tuple(spread(i, A_BITS) for i in range(4))
B_MASKS = tuple(spread(i, B_BITS) for i in range(4))
SLOTS = tuple(b | a for b in B_MASKS for a in A_MASKS)


def gather_bits(number, bits):
    return sum(((number >> b) & 1) << i for i, b in enumerate(bits))


def flip(value, mask):
    count = lax.axis_size("sp")
    return lax.ppermute(value, "sp", [(i, i ^ mask) for i in range(count)])


def other_core(value):
    return lax.ppermute(value, "tp", [(0, 1), (1, 0)])


def vmem():
    return pl.BlockSpec(memory_space=pltpu.VMEM)


def smem():
    return pl.BlockSpec(memory_space=pltpu.SMEM)


def call(kernel, outs, ins, scratch=(), name=None, flops=0):
    return pl.pallas_call(
        kernel,
        out_shape=outs,
        in_specs=[smem()] + [vmem()] * (len(ins) - 1),
        out_specs=jax.tree.map(lambda _: vmem(), outs),
        scratch_shapes=list(scratch),
        name=name,
        cost_estimate=pl.CostEstimate(flops=flops, transcendentals=0, bytes_accessed=1 << 20),
        compiler_params=pltpu.CompilerParams(vmem_limit_bytes=58 << 20),
    )(*ins)


def lanes_at(block):
    return pl.ds(pl.multiple_of(block * LANES, LANES), LANES)


def prep_kernel(who, q_ref, k_ref, v_ref, qg_ref, kg_ref, cos_ref, sin_ref, *rest):
    outs, (q_scr, k_scr) = rest[:4], rest[4:]
    rows = q_ref.shape[0]
    lane = lax.broadcasted_iota(jnp.int32, (rows, LANES), 1)
    low16 = (lane & 31) < 16
    own = lax.broadcasted_iota(jnp.int32, (LANES, LANES), 0) // HEAD_DIM
    same = own == lax.broadcasted_iota(jnp.int32, (LANES, LANES), 1) // HEAD_DIM
    mean = jnp.where(same, 1.0 / HEAD_DIM, 0.0).astype(F32)
    cos, sin = cos_ref[...], sin_ref[...]

    def turned(pair, gain):
        x = pair.astype(F32)
        power = jnp.dot(x * x, mean, precision=lax.Precision.HIGHEST, preferred_element_type=F32)
        y = x * lax.rsqrt(power + NORM_EPS) * gain
        near = jnp.where(low16, pltpu.roll(y, LANES - 16, 1), pltpu.roll(y, 16, 1))
        return y * cos + near * sin

    for i in range(q_ref.shape[1] // LANES):
        at = slice(i * LANES, (i + 1) * LANES)
        q_scr[:, at] = (turned(q_ref[:, at], qg_ref[...]) * HEAD_DIM**-0.5).astype(BF16)
    for i in range(k_ref.shape[1] // LANES):
        at = slice(i * LANES, (i + 1) * LANES)
        k_scr[:, at] = turned(k_ref[:, at], kg_ref[...])
    for d, out in enumerate(outs):
        share = who[0] ^ d
        out[:, :LANES] = q_scr[:, lanes_at(share)]
        keys = k_scr[:, lanes_at(share >> 1)]
        values = v_ref[:, lanes_at(share >> 1)].astype(F32)
        odd = (share & 1) == 1
        keys = jnp.where(odd, pltpu.roll(keys, HEAD_DIM, 1), keys)
        values = jnp.where(odd, values, pltpu.roll(values, HEAD_DIM, 1))
        out[:, LANES:] = jnp.where(lane < HEAD_DIM, keys, values).astype(BF16)


def attend_kernel(who, *refs):
    packed, kvs = refs[:4], refs[4:8]
    outs, ones_scr = refs[8:10], refs[10]
    half = packed[0].shape[0] // 2
    span = kvs[0].shape[0]
    lane = lax.broadcasted_iota(jnp.int32, (half, LANES), 1)
    wide = lax.broadcasted_iota(jnp.int32, (span, LANES), 1)
    for j, kv in enumerate(kvs):
        ones_scr[j] = jnp.where(wide < HEAD_DIM, jnp.ones((), BF16), kv[...])
    for s in range(4):
        for h in range(2):
            row = pl.multiple_of((who[1] ^ h) * half, half)
            q = packed[s][pl.ds(row, half), :LANES].astype(F32)
            first = jnp.where(lane < HEAD_DIM, q, 0.0)
            second = jnp.where(lane < HEAD_DIM, pltpu.roll(q, HEAD_DIM, 1), 0.0)
            both = jnp.concatenate([first, second], axis=0).astype(BF16)
            scores = [
                lax.dot_general(both, kv[...], (((1,), (1,)), ((), ())), preferred_element_type=F32)
                for kv in kvs
            ]
            top = functools.reduce(
                jnp.maximum, [jnp.max(x, axis=1, keepdims=True) for x in scores]
            )
            total = jnp.zeros((2 * half, LANES), F32)
            for j, x in enumerate(scores):
                weights = jnp.exp(x - top).astype(BF16)
                total = total + jnp.dot(weights, ones_scr[j], preferred_element_type=F32)
            share = total / pltpu.roll(total, HEAD_DIM, 1)
            first = pltpu.roll(share[:half], HEAD_DIM, 1)
            outs[h][s * half : (s + 1) * half, :] = jnp.where(
                lane < HEAD_DIM, first, share[half:]
            ).astype(BF16)


def mix_kernel(who, *refs):
    atts, residuals = refs[:4], refs[4:8]
    w_own, w_other, gain, updated, normed, own_scr, other_scr, up_scr = refs[8:]
    half = residuals[0].shape[0]
    width = up_scr.shape[1]
    for d, att in enumerate(atts):
        at = lanes_at(who[0] ^ d)
        for b in range(4):
            here, there = (slice(x * half, (x + 1) * half) for x in (b, b ^ d))
            own_scr[here, at] = att[there, :LANES]
            other_scr[here, at] = att[there, LANES:]
    step = 512
    power = jnp.zeros((4 * half, 1), F32)
    for n in range(0, width, step):
        at = slice(n, n + step)
        parts = [
            jnp.dot(x[...], w[:, at], preferred_element_type=F32).astype(BF16).astype(F32)
            for x, w in ((own_scr, w_own), (other_scr, w_other))
        ]
        mixed = (parts[0] + parts[1]).astype(BF16).astype(F32)
        residual = jnp.concatenate([r[:, at] for r in residuals], axis=0).astype(F32)
        rows = (residual + mixed).astype(BF16)
        up_scr[:, at] = rows
        values = rows.astype(F32)
        power = power + jnp.sum(values * values, axis=1, keepdims=True)
    scale = lax.rsqrt(power / width + NORM_EPS)
    updated[...] = up_scr[:half, :]
    for i, d in enumerate(SLOTS):
        at = lanes_at(who[2] ^ d)
        normed[:, i * LANES : (i + 1) * LANES] = (
            up_scr[:, at].astype(F32) * scale * gain[:, at]
        ).astype(BF16)


def up_kernel(who, n_own, n_other, *refs):
    weights, out = refs[:4], refs[4]
    half = n_own.shape[0] // 4
    depth = weights[0].shape[0]
    for h, x in enumerate((n_own, n_other)):
        total = None
        for b, w in enumerate(weights):
            part = jnp.dot(
                x[:, b * depth : (b + 1) * depth], w[...], preferred_element_type=F32
            )
            total = part if total is None else total + part
        rows = total.astype(BF16)
        for s in range(4):
            at = pl.multiple_of(s * 2 * half + (who[1] ^ h) * half, half)
            out[pl.ds(at, half), :] = rows[s * half : (s + 1) * half]


def down_kernel(who, up, edges, taps_v, taps_g, *refs):
    weights, outs, hid = refs[:4], refs[4:6], refs[6]
    rows = up.shape[0] // 4
    units = taps_v.shape[1]
    half = rows // 2
    at_row = lax.broadcasted_iota(jnp.int32, (rows, units), 0)

    def conv(s, at, taps):
        x = up[s * rows : (s + 1) * rows, at].astype(F32)
        left = edges[pl.ds(who[4 + 2 * s], 1), at]
        right = edges[pl.ds(who[5 + 2 * s], 1), at]
        before = jnp.where(at_row == 0, left, pltpu.roll(x, 1, 0))
        after = jnp.where(at_row == rows - 1, right, pltpu.roll(x, rows - 1, 0))
        return before * taps[0:1, :] + x * taps[1:2, :] + after * taps[2:3, :]

    for s in range(4):
        value = conv(s, slice(0, units), taps_v)
        gate = conv(s, slice(units, 2 * units), taps_g)
        hid[s * rows : (s + 1) * rows, :] = (
            jax.nn.gelu(gate, approximate=True) * value
        ).astype(BF16)
    width = weights[0].shape[1]
    for h in range(2):
        x = jnp.concatenate(
            [
                hid[pl.ds(pl.multiple_of(s * rows + (who[1] ^ h) * half, half), half), :]
                for s in range(4)
            ],
            axis=0,
        )
        for b, w in enumerate(weights):
            outs[h][:, b * width : (b + 1) * width] = jnp.dot(
                x, w[...], preferred_element_type=F32
            ).astype(BF16)


def final_kernel(who, updated, own, *refs):
    others, out = refs[:3], refs[3]
    for i, d in enumerate(SLOTS):
        total = own[:, i * LANES : (i + 1) * LANES].astype(F32)
        for e, other in enumerate(others, 1):
            j = i ^ e
            total = total + other[:, j * LANES : (j + 1) * LANES].astype(F32)
        branch = total.astype(BF16).astype(F32)
        at = lanes_at(who[2] ^ d)
        out[:, at] = (updated[:, at].astype(F32) + branch).astype(BF16)


def grouped_shards(
    query_proj,
    key_proj,
    value_proj,
    q_gain,
    k_gain,
    residual,
    out_weight,
    norm_gain,
    value_weight,
    gate_weight,
    down_weight,
    conv_value,
    conv_gate,
):
    tokens = query_proj.shape[0]
    half = tokens // 2
    width = residual.shape[1]
    units = value_weight.shape[1] // 4
    sp, core = lax.axis_index("sp"), lax.axis_index("tp")
    group = gather_bits(sp, A_BITS)
    count = lax.axis_size("sp")
    shape = jax.ShapeDtypeStruct

    reach = sorted({gather_bits(m, B_BITS) for m in ((1 << k) - 1 for k in range(1, count.bit_length()))})
    index = []
    for d in A_MASKS:
        block = sp ^ d
        for side, step in ((1, -1), (0, 1)):
            there = block + step
            changed = block ^ there
            source = gather_bits(changed, B_BITS)
            place = sum(jnp.where(source == r, n, 0) for n, r in enumerate(reach))
            slot = gather_bits(changed ^ d, A_BITS)
            row = 8 * place + 2 * slot + side
            inside = (there >= 0) & (there < count)
            index.append(jnp.where(inside, row, 8 * len(reach)))
    who = jnp.stack([group, core, sp, sp] + index).astype(jnp.int32)

    t = sp * tokens + lax.broadcasted_iota(jnp.int32, (tokens, LANES), 0)
    lane = lax.broadcasted_iota(jnp.int32, (tokens, LANES), 1)
    where = jnp.where(lane % HEAD_DIM < HEAD_DIM // 2, t // GRID_W, t % GRID_W).astype(F32)
    quarter = HEAD_DIM // 4
    power = (2 * (lane % quarter)).astype(F32) / (HEAD_DIM // 2)
    angle = where * ROPE_BASE ** (-power)
    cos = jnp.cos(angle)
    sin = jnp.where(lane % (2 * quarter) < quarter, -jnp.sin(angle), jnp.sin(angle))

    def shares(weight, axis):
        return [
            lax.dynamic_slice_in_dim(weight, (group ^ d) * units, units, axis) for d in range(4)
        ]

    packs = call(
        prep_kernel,
        [shape((tokens, 2 * LANES), BF16)] * 4,
        (
            who,
            query_proj,
            key_proj,
            value_proj,
            jnp.tile(q_gain, 2)[None, :],
            jnp.tile(k_gain, 2)[None, :],
            cos,
            sin,
        ),
        scratch=[
            pltpu.VMEM(query_proj.shape, BF16),
            pltpu.VMEM(key_proj.shape, F32),
        ],
        name="prep",
        flops=10**8,
    )
    packs = [packs[0]] + [flip(packs[d], A_MASKS[d]) for d in range(1, 4)]

    ups = [
        jnp.concatenate(pair, axis=1)
        for pair in zip(shares(value_weight, 1), shares(gate_weight, 1))
    ]
    ups = [ups[0]] + [flip(ups[d], A_MASKS[d]) for d in range(1, 4)]
    up_own = jnp.concatenate(ups, axis=0)

    kv_own = jnp.concatenate([p[:, LANES:] for p in packs], axis=0)
    first, second = B_MASKS[1], B_MASKS[2]
    kv_z = flip(kv_own, second)
    kv_y = flip(kv_own, first)
    kv_yz = flip(kv_z, first)

    up_z = flip(up_own, second)
    up_y = flip(up_own, first)
    up_yz = flip(up_z, first)

    out_other = other_core(out_weight)

    mine = lax.dynamic_slice_in_dim(residual, core * half, half, 0)
    residuals = [mine] + [flip(mine, A_MASKS[d]) for d in range(1, 4)]

    downs = shares(down_weight, 0)
    downs = [downs[0]] + [flip(downs[d], A_MASKS[d]) for d in range(1, 4)]
    down_own = jnp.concatenate(downs, axis=1)
    down_z = flip(down_own, second)
    down_y = flip(down_own, first)
    down_yz = flip(down_z, first)

    span = kv_own.shape[0]
    att_own, att_send = call(
        attend_kernel,
        [shape((4 * half, LANES), BF16)] * 2,
        (who, *packs, kv_own, kv_y, kv_z, kv_yz),
        scratch=[pltpu.VMEM((4, span, LANES), BF16)],
        name="attend",
        flops=10**10,
    )
    att_other = other_core(att_send)
    att = jnp.concatenate([att_own, att_other], axis=1)
    atts = [att] + [flip(att, A_MASKS[d]) for d in range(1, 4)]

    updated, n_own = call(
        mix_kernel,
        [shape((half, width), BF16), shape((4 * half, width), BF16)],
        (who, *atts, *residuals, out_weight, out_other, norm_gain[None, :]),
        scratch=[
            pltpu.VMEM((4 * half, 4 * LANES), BF16),
            pltpu.VMEM((4 * half, 4 * LANES), BF16),
            pltpu.VMEM((4 * half, width), BF16),
        ],
        name="mix",
        flops=3 * 10**9,
    )
    n_other = other_core(n_own)

    up = call(
        up_kernel,
        shape((4 * tokens, 2 * units), BF16),
        (who, n_own, n_other, up_own, up_y, up_z, up_yz),
        name="up",
        flops=5 * 10**9,
    )
    edge = up.reshape(4, tokens, 2 * units)[:, :: tokens - 1].reshape(8, 2 * units)
    edges = [edge] + [flip(edge, B_MASKS[r]) for r in reach if r]
    edges = jnp.concatenate(edges + [jnp.zeros_like(edge)], axis=0).astype(F32)

    part_own, part_send = call(
        down_kernel,
        [shape((4 * half, width), BF16)] * 2,
        (
            who,
            up,
            edges,
            lax.dynamic_slice_in_dim(conv_value, group * units, units, 1),
            lax.dynamic_slice_in_dim(conv_gate, group * units, units, 1),
            down_own,
            down_y,
            down_z,
            down_yz,
        ),
        scratch=[pltpu.VMEM((4 * tokens, units), BF16)],
        name="down",
        flops=3 * 10**9,
    )
    part = (part_own.astype(F32) + other_core(part_send).astype(F32)).astype(BF16)
    parts = [part[d * half : (d + 1) * half] for d in range(4)]
    parts = [parts[0]] + [flip(parts[d], A_MASKS[d]) for d in range(1, 4)]
    return call(
        final_kernel,
        shape((half, width), BF16),
        (who, updated, *parts),
        name="final",
        flops=10**7,
    )


def padded_2(shard, sides, width):
    for axis, dim in sides:
        count, length = (lax.axis_size(axis), shard.shape[dim])
        up = [(i, (i + 1) % count) for i in range(count - 1)]
        down = [(j, i) for i, j in up]
        last = lax.slice_in_dim(shard, length - width, length, axis=dim)
        first = lax.slice_in_dim(shard, 0, width, axis=dim)
        before = lax.ppermute(last, axis, up)
        after = lax.ppermute(first, axis, down)
        shard = jnp.concatenate([before, shard, after], axis=dim)
    return shard


def rms_norm(block_in, gain_vec):
    values = block_in.astype(jnp.float32)
    inv_rms = lax.rsqrt(jnp.mean(values * values, axis=-1, keepdims=True) + NORM_EPS)
    return values * inv_rms * gain_vec


def rotate_half(values, position):
    full_width = values.shape[-1]
    half_width = full_width // 2
    frequency = ROPE_BASE ** (-jnp.arange(0, full_width, 2, dtype=jnp.float32) / full_width)
    angles = position.astype(jnp.float32)[:, None] * frequency[None, :]
    cosine = jnp.cos(angles)[:, None, :]
    sine_part = jnp.sin(angles)[:, None, :]
    first_half = values[..., :half_width]
    second_half = values[..., half_width:]
    return jnp.concatenate(
        [
            first_half * cosine - second_half * sine_part,
            first_half * sine_part + second_half * cosine,
        ],
        axis=-1,
    )


def grid_rotary(values, positions):
    half_width = values.shape[-1] // 2
    grid_row = positions // GRID_W
    column = positions % GRID_W
    return jnp.concatenate(
        [
            rotate_half(values[..., :half_width], grid_row),
            rotate_half(values[..., half_width:], column),
        ],
        axis=-1,
    )


def attend_piece(state_in, key_piece, queries):
    row_total = key_piece.shape[0]
    kv_count = queries.shape[0]
    head_width = queries.shape[3]
    key_span = 1024
    blocks_count = row_total // key_span
    keys_all = key_piece[:, : kv_count * head_width].reshape(
        blocks_count, key_span, kv_count, head_width
    )
    values_all = key_piece[:, kv_count * head_width :].reshape(
        blocks_count, key_span, kv_count, head_width
    )

    def advance(state, blocks_in):
        run_max, run_sum, run_acc = state
        key_block, value_block = blocks_in
        scores = jnp.einsum(
            "kgqd,skd->kgqs", queries, key_block, preferred_element_type=jnp.float32
        )
        new_max = jnp.maximum(run_max, jnp.max(scores, axis=-1))
        weights = jnp.exp(scores - new_max[..., None])
        shrink = jnp.exp(run_max - new_max)
        run_sum = run_sum * shrink + jnp.sum(weights, axis=-1)
        run_acc = run_acc * shrink[..., None] + jnp.einsum(
            "kgqs,skd->kgqd",
            weights.astype(jnp.bfloat16),
            value_block,
            preferred_element_type=jnp.float32,
        )
        return ((new_max, run_sum, run_acc), None)

    final_state, ignored = lax.scan(advance, state_in, (keys_all, values_all))
    return final_state


def general_shards(
    query_proj,
    key_proj,
    value_proj,
    q_gain,
    k_gain,
    residual,
    out_weight,
    norm_gain,
    value_weight,
    gate_weight,
    down_weight,
    conv_value,
    conv_gate,
):
    tokens = query_proj.shape[0]
    heads_here = query_proj.shape[1] // HEAD_DIM
    kv_here = key_proj.shape[1] // HEAD_DIM
    group_size = heads_here // kv_here
    offset = lax.axis_index("sp") * tokens
    positions = offset + jnp.arange(tokens, dtype=jnp.int32)
    down_whole = lax.all_gather(down_weight, "sp", axis=1, tiled=True)
    queries = grid_rotary(
        rms_norm(query_proj.reshape(tokens, heads_here, HEAD_DIM), q_gain), positions
    ) * HEAD_DIM ** (-0.5)
    queries = (
        queries.astype(jnp.bfloat16)
        .reshape(tokens, kv_here, group_size, HEAD_DIM)
        .transpose(1, 2, 0, 3)
    )
    keys_rot = grid_rotary(
        rms_norm(key_proj.reshape(tokens, kv_here, HEAD_DIM), k_gain), positions
    ).astype(jnp.bfloat16)
    packed = jnp.concatenate([keys_rot.reshape(tokens, kv_here * HEAD_DIM), value_proj], axis=1)
    start_state = (
        jnp.full((kv_here, group_size, tokens), -1e30, jnp.float32),
        jnp.zeros((kv_here, group_size, tokens), jnp.float32),
        jnp.zeros((kv_here, group_size, tokens, HEAD_DIM), jnp.float32),
    )
    run_max, run_sum, run_acc = attend_piece(
        start_state, lax.all_gather(packed, "sp", axis=0, tiled=True), queries=queries
    )
    attended = (
        (run_acc / run_sum[..., None])
        .transpose(2, 0, 1, 3)
        .reshape(tokens, heads_here * HEAD_DIM)
        .astype(jnp.bfloat16)
    )
    row_share = tokens // lax.axis_size("tp")
    row_start = lax.axis_index("tp") * row_share
    mix_out = lax.psum(
        jnp.dot(attended, out_weight, preferred_element_type=jnp.float32).astype(jnp.bfloat16), "tp"
    )
    whole_rows = (residual.astype(jnp.float32) + mix_out.astype(jnp.float32)).astype(jnp.bfloat16)
    normed = rms_norm(whole_rows, norm_gain).astype(jnp.bfloat16)
    updated = lax.dynamic_slice_in_dim(whole_rows, row_start, row_share, 0)
    value_up = jnp.dot(
        normed,
        lax.all_gather(value_weight, "sp", axis=0, tiled=True),
        preferred_element_type=jnp.float32,
    )
    gate_up = jnp.dot(
        normed,
        lax.all_gather(gate_weight, "sp", axis=0, tiled=True),
        preferred_element_type=jnp.float32,
    )
    stacked = jnp.stack([value_up.astype(jnp.bfloat16), gate_up.astype(jnp.bfloat16)])
    padded = padded_2(stacked, (("sp", 1),), 1).astype(jnp.float32)
    conv_val = (
        padded[0, :-2] * conv_value[0]
        + padded[0, 1:-1] * conv_value[1]
        + padded[0, 2:] * conv_value[2]
    )
    conv_gated = (
        padded[1, :-2] * conv_gate[0]
        + padded[1, 1:-1] * conv_gate[1]
        + padded[1, 2:] * conv_gate[2]
    )
    hidden = (jax.nn.gelu(conv_gated, approximate=True) * conv_val).astype(jnp.bfloat16)
    branch = lax.psum_scatter(
        jnp.dot(hidden, down_whole, preferred_element_type=jnp.float32).astype(jnp.bfloat16),
        "tp",
        scatter_dimension=0,
        tiled=True,
    )
    return (updated.astype(jnp.float32) + branch.astype(jnp.float32)).astype(jnp.bfloat16)


def shards(query_proj, key_proj, value_proj, q_gain, k_gain, residual, *rest):
    tokens, queries = query_proj.shape
    units, model = rest[2].shape[1], residual.shape[1]
    count = lax.axis_size("sp")
    fits = (
        count == 1 << len(A_BITS + B_BITS)
        and lax.axis_size("tp") == 2
        and queries == 4 * LANES
        and key_proj.shape[1] == 2 * LANES
        and tokens % 256 == 0
        and units % (4 * LANES) == 0
        and model == count * LANES
    )
    body = grouped_shards if fits else general_shards
    return body(query_proj, key_proj, value_proj, q_gain, k_gain, residual, *rest)


def solution(mesh):
    return jax.shard_map(
        shards,
        mesh=mesh,
        in_specs=(
            P("sp", "tp"),
            P("sp", "tp"),
            P("sp", "tp"),
            P(),
            P(),
            P("sp", None),
            P("tp", None),
            P(),
            P("sp", "tp"),
            P("sp", "tp"),
            P("tp", "sp"),
            P(None, "tp"),
            P(None, "tp"),
        ),
        out_specs=P(("sp", "tp"), None),
        check_vma=False,
    )
```
